512 devices in a mesh: sp: 32 (over z, core), tp: 16 (over y, x).
Axes of the slice: x: 4, y: 4, z: 16, core: 2. Of those that a mesh axis runs over, the one named last changes fastest.
Arguments:
- residual_in: bfloat16 [8192, 2048], P('sp', 'tp'), may hold values from -20 to 20
- conv_value: bfloat16 [8192, 2048], P('sp', 'tp'), may hold values from -6 to 6
- conv_gate: bfloat16 [8192, 2048], P('sp', 'tp'), may hold values from -9 to 9
- doc_ids: int32 [8192], P('sp'), may hold values from 0 to 15, never falling along the last dimension, each value on 1 to 1024 neighbouring positions
- conv_kernel: bfloat16 [31, 2048], P(None, 'tp'), may hold values from -3 to 3
- ln_gain: bfloat16 [2048], P('tp'), may hold values from 0.099609375 to 1.8984375
- out_weight: bfloat16 [2048, 2048], P(None, 'tp'), may hold values from -0.25 to 0.25
- norm_gain: bfloat16 [2048], P('tp'), may hold values from 0.099609375 to 1.8984375
- routes: int32 [8192, 2], P('sp'), may hold values from 0 to 31, all different within a row; in each aligned block of 256 rows (0 to 255, 256 to 511, ...) at most 32 rows name the same one
- route_weight: float32 [8192, 2], P('sp'), may hold values from 0.1 to 1
- gate_w: bfloat16 [32, 2048, 4096], P('sp', None, 'tp'), may hold values from -0.125 to 0.125
- up_w: bfloat16 [32, 2048, 4096], P('sp', None, 'tp'), may hold values from -0.125 to 0.125
- down_w: bfloat16 [32, 4096, 2048], P('sp', 'tp'), may hold values from -0.125 to 0.125
Outputs:
- mixed: bfloat16 [8192, 2048], P('sp', 'tp')
The draws below stay inside these ranges and needn't reach their ends.
Inputs may be any that keep to these rules, and one draw needn't show every extreme that they name: `routes`: in each aligned block of 256 positions no expert is named by more than 32 positions, a bound that some block reaches; a position's two experts differ. `doc_ids`: never falls along the positions; each document spans 1 to 1024 positions, one exactly that many.
All inputs are finite; a program needn't handle non-finite values.
Results may differ from the reference program's by a relative error of at most 0.012.
Values may be sent and summed in bfloat16 or wider, within the bound.
No kernel may reach another device: no remote copies, remote signals or barrier semaphores. Data moves between devices by JAX's collectives and lax.ppermute only.
A program may use at most 64 MiB of HBM per device.

```python
import math
import jax
import jax.numpy as jnp
import numpy as np
from jax import lax

D = 2048
C = 2048
FE = 4096
KW = 31
TOK_SP = 256
TOKENS = 8192
EXPERTS = 32
CAP = 32
N_SP = 32
N_TP = 16


def draw_residual_in(key, part):
    column = jnp.arange(D, dtype=jnp.float32) / D
    scale = 0.3 * 10.0 ** column
    base = jnp.clip(jax.random.normal(key, (TOKENS, D), jnp.float32), -6.0, 6.0)
    return (base * scale).astype(jnp.bfloat16)


def draw_conv_kernel(key, part):
    channel = jnp.arange(C, dtype=jnp.float32) / C
    scale = KW ** (-0.5) * 10.0 ** channel / 3.0
    base = jnp.clip(jax.random.normal(key, (KW, C), jnp.float32), -4.0, 4.0)
    return (base * scale).astype(jnp.bfloat16)


def strengthened(array, own_key, source, target, blocks, factor):
    owner, partner = [(jnp.arange(array.shape[dim]) // (array.shape[dim] // blocks)).reshape([-1 if axis == dim else 1 for axis in range(array.ndim)]) for dim in (source, target)]
    chosen = jax.random.permutation(own_key, blocks)[partner]
    strong = (owner == chosen) | (owner == (partner + blocks // 2) % blocks)
    return jnp.where(strong, factor * array, array)


def levels(own_key, extent, shards, least, top_value):
    def one(dim, shards_of):
        heights = jax.random.uniform(jax.random.fold_in(jax.random.fold_in(own_key, 6), dim), (shards_of,), jnp.float32, least / len(shards), top_value / len(shards))
        return jnp.repeat(jnp.exp(heights), extent[dim] // shards_of).reshape((-1,) + (1,) * (len(extent) - dim - 1))

    gain = one(*shards[0])
    for cut in shards[1:]:
        gain = gain * one(*cut)
    return gain


def length_profile(amount, total, bound, skew):
    portions = [(1 << 20) // math.isqrt(grade ** skew) + 1 for grade in range(2, amount + 1)]
    spare, given = total - bound - (amount - 1), [1] * (amount - 1)
    while spare > 0:
        free = [i for i in range(amount - 1) if given[i] < bound]
        whole, left = sum([portions[i] for i in free]), spare
        for i in free:
            extra = min(bound - given[i], max(1, left * portions[i] // whole), spare)
            given[i] = given[i] + extra
            spare = spare - extra
    return np.array([bound] + given)


def uneven(stream_key, amount, total, bound, lean):
    if amount == 2:
        one = jax.random.randint(stream_key, (), max(1, total - bound), min(bound, total - 1) + 1)
        return jnp.stack([one, total - one])
    tallies = jnp.asarray(length_profile(amount, total, bound, lean), jnp.int32)
    couples = (amount - 1) // 2
    source_of, receiver = tallies[1:1 + 2 * couples:2], tallies[2:2 + 2 * couples:2]
    room = jnp.minimum(source_of - 1, bound - receiver)
    passed = jax.random.randint(jax.random.fold_in(stream_key, 1), (couples,), 0, 1 << 20) % (room + 1)
    tallies = tallies.at[1:1 + 2 * couples:2].set(source_of - passed).at[2:2 + 2 * couples:2].set(receiver + passed)
    return tallies[jax.random.permutation(jax.random.fold_in(stream_key, 2), amount)]


def routed_block(key, own, number, rows, number_of, top, most, lean):
    ranking = jax.random.permutation(key, number_of)
    crowded, usual = shares(number_of, rows * top, most, lean, True), shares(number_of, rows * top, most, lean, False)
    places = jnp.arange(number_of)

    def named(sizes, turn):
        used = int((sizes > 0).sum())
        fixed = max(1, used // 4)
        shifted = fixed + (places - fixed + turn * (used - fixed)) % max(1, number_of - fixed)
        return jnp.zeros((number_of,), jnp.int32).at[ranking[jnp.where(places < fixed, places, shifted)]].set(jnp.asarray(sizes, jnp.int32))

    sizes = jnp.where(number % 4 == 0, named(crowded, number // 4), named(usual, number - number // 4 - 1))
    mixed = jax.random.permutation(jax.random.fold_in(own, 3), number_of)
    source_of, receiver = mixed[0:number_of // 2 * 2:2], mixed[1:number_of // 2 * 2:2]
    margin = jnp.minimum(sizes[source_of] - 1, most - sizes[receiver]) // 2
    margin = jnp.where((source_of == ranking[0]) | (receiver == ranking[0]) | (sizes[receiver] == 0), 0, jnp.maximum(margin, 0))
    shifted = jax.random.randint(jax.random.fold_in(own, 4), (number_of // 2,), 0, 1 << 20) % (margin + 1)
    sizes = sizes.at[source_of].add(-shifted).at[receiver].add(shifted)
    labels = jnp.searchsorted(jnp.cumsum(sizes), jnp.arange(rows * top), side="right").astype(jnp.int32)
    listing = labels.reshape(top, rows).T
    listing = listing[jax.random.permutation(jax.random.fold_in(own, 1), rows)]
    turn = jax.random.randint(jax.random.fold_in(own, 2), (rows, 1), 0, top)
    return jnp.take_along_axis(listing, (jnp.arange(top)[None, :] + turn) % top, axis=1)


def shares(amount, total, reach, lean, full):
    weights = [(1 << 20) // math.isqrt(grade ** lean) + 1 for grade in range(1, amount + 1)]
    largest = reach if full else min(reach, max(-(-total // amount), total * weights[0] // sum(weights)))
    least = 1 if total - largest >= amount - 1 else 0
    counts, rest = [largest] + [least] * (amount - 1), total - largest - least * (amount - 1)
    while rest > 0:
        movable = [i for i in range(1, amount) if counts[i] < largest] or [i for i in range(1, amount) if counts[i] < reach]
        mass, remaining = sum([weights[i] for i in movable]), rest
        for i in movable:
            more = min(reach - counts[i], max(1, remaining * weights[i] // mass), rest)
            counts[i] = counts[i] + more
            rest = rest - more
    return np.array(counts)


def scatter_about(stream_key, dims, width, most, cuts=(), kind=jnp.bfloat16):
    gain = levels(stream_key, dims, cuts, -0.22, 0.18) if cuts else 1.0
    drawn = jax.random.normal(stream_key, dims, jnp.float32) * width * gain
    return jnp.minimum(jnp.maximum(drawn, -most), most).astype(kind)


def bell_draw_with(own_key, dims, deviation, reach, pieces, heavy, kind=jnp.bfloat16):
    drawn = deviation * jax.random.normal(own_key, dims, jnp.float32)
    if pieces:
        drawn = drawn * levels(own_key, dims, pieces, -0.22, 0.18)
    return jnp.clip(strengthened(drawn, jax.random.fold_in(own_key, 3), *heavy), -reach, reach).astype(kind)


def setup_inputs(seed: int = 0) -> dict:
    key_list = jax.random.split(jax.random.key(seed), 14)
    residual_in = draw_residual_in(jax.random.fold_in(key_list[13], 71), 0)
    conv_value = scatter_about(key_list[1], (TOKENS, C), 1.0, 6.0, ((0, 32), (1, 16)))
    conv_gate = scatter_about(key_list[2], (TOKENS, C), 1.5, 9.0, ((0, 32), (1, 16)))
    doc_ids = jnp.searchsorted(jnp.cumsum(uneven(key_list[3], N_SP // 2, TOKENS, 4 * TOK_SP, 0)), jnp.arange(TOKENS), side="right").astype(jnp.int32)
    conv_kernel = draw_conv_kernel(jax.random.fold_in(key_list[13], 71), 0)
    ln_gain = jnp.clip(1.0 + 0.18 * jax.random.normal(key_list[5], (C,), jnp.float32), 0.099609375, 1.8984375).astype(jnp.bfloat16)
    out_weight = scatter_about(key_list[6], (C, D), (C // 4) ** -0.5, 0.25, ((1, 16),))
    norm_gain = jnp.clip(1.0 + 0.18 * jax.random.normal(key_list[7], (D,), jnp.float32), 0.099609375, 1.8984375).astype(jnp.bfloat16)
    routes_keys = jax.random.split(jax.random.fold_in(key_list[8], 1), TOKENS // TOK_SP)
    routes_turns = jax.random.permutation(jax.random.fold_in(key_list[8], 3), TOKENS // TOK_SP)
    routes = jax.vmap(lambda own, number: routed_block(jax.random.fold_in(key_list[8], 2), own, number, TOK_SP, EXPERTS, 2, CAP, 1))(routes_keys, routes_turns).reshape((TOKENS, 2))
    route_weight = jnp.clip(jnp.exp(math.log(1.0) - 2.3025851 * jax.random.uniform(key_list[9], (TOKENS, 2), jnp.float32) ** levels(key_list[9], (TOKENS, 2), ((0, 32),), -0.2, 0.2)), 0.1, 1.0)
    gate_w = scatter_about(key_list[10], (EXPERTS, D, FE), D ** -0.5, 0.125, ((0, 32), (2, 16)))
    up_w = scatter_about(key_list[11], (EXPERTS, D, FE), D ** -0.5, 0.125, ((0, 32), (2, 16)))
    down_w = bell_draw_with(key_list[12], (EXPERTS, FE, D), FE ** -0.5, 0.125, ((0, 32), (1, 16)), (1, 2, 16, 2.0))
    return {"residual_in": residual_in, "conv_value": conv_value, "conv_gate": conv_gate, "doc_ids": doc_ids, "conv_kernel": conv_kernel, "ln_gain": ln_gain, "out_weight": out_weight, "norm_gain": norm_gain, "routes": routes, "route_weight": route_weight, "gate_w": gate_w, "up_w": up_w, "down_w": down_w}


epsilon = 1e-06

def reference(residual_in, conv_value, conv_gate, doc_ids, conv_kernel, ln_gain, out_weight, norm_gain, routes, route_weight, gate_w, up_w, down_w):
    gated = (conv_value.astype(jnp.float32) * jax.nn.sigmoid(conv_gate.astype(jnp.float32))).astype(jnp.bfloat16)
    positions = gated.shape[0]
    lookback = KW - 1
    padded = jnp.concatenate([jnp.zeros((lookback, C), jnp.bfloat16), gated], 0)
    doc_padded = jnp.concatenate([jnp.full((lookback,), -1, jnp.int32), doc_ids], 0)
    kernel = conv_kernel.astype(jnp.float32)
    conv_out = jnp.zeros((positions, C), jnp.float32)
    for kernel_tap in range(KW):
        same_doc = (doc_padded[kernel_tap:kernel_tap + positions] == doc_ids)[:, None]
        conv_out = conv_out + jnp.where(same_doc, padded[kernel_tap:kernel_tap + positions].astype(jnp.float32) * kernel[kernel_tap], 0.0)
    chan_mean = lax.optimization_barrier(jnp.mean(conv_out, 1, keepdims=True))
    chan_square = lax.optimization_barrier(jnp.mean(conv_out * conv_out, 1, keepdims=True))
    activated = jax.nn.silu((conv_out - chan_mean) * lax.rsqrt(chan_square - chan_mean * chan_mean + epsilon) * ln_gain.astype(jnp.float32)).astype(jnp.bfloat16)
    projected = jnp.dot(activated, out_weight, preferred_element_type=jnp.float32).astype(jnp.bfloat16)
    stream = (residual_in.astype(jnp.float32) + projected.astype(jnp.float32)).astype(jnp.bfloat16)
    stream_f = stream.astype(jnp.float32)
    normed = (stream_f * lax.rsqrt(lax.optimization_barrier(jnp.mean(stream_f * stream_f, 1, keepdims=True)) + epsilon) * norm_gain.astype(jnp.float32)).astype(jnp.bfloat16)
    capacity = 4 * TOK_SP // EXPERTS
    flat_routes = routes.reshape(N_SP, TOK_SP * 2)
    onehot = (flat_routes[:, :, None] == jnp.arange(EXPERTS, dtype=jnp.int32)).astype(jnp.int32)
    slot_rank = lax.optimization_barrier(jnp.sum((jnp.cumsum(onehot, 1) - onehot) * onehot, 2)).astype(jnp.int32)
    token_local = jnp.arange(TOK_SP * 2, dtype=jnp.int32) // 2
    block_start = (jnp.arange(N_SP, dtype=jnp.int32) * TOK_SP)[:, None]
    token_global = token_local[None, :] + block_start
    slot_token = jnp.full((N_SP, EXPERTS * capacity), positions, jnp.int32)
    slot_token = slot_token.at[jnp.arange(N_SP, dtype=jnp.int32)[:, None], flat_routes * capacity + slot_rank].set(token_global)
    slot_token = slot_token.reshape(N_SP, EXPERTS, capacity).transpose(1, 0, 2).reshape(EXPERTS, N_SP * capacity)

    def expert(operands):
        chosen, weight_gate, weight_up, weight_down = operands
        gathered = jnp.take(normed, chosen, axis=0, mode='fill', fill_value=0)
        hidden = (jax.nn.silu(jnp.dot(gathered, weight_gate, preferred_element_type=jnp.float32)) * jnp.dot(gathered, weight_up, preferred_element_type=jnp.float32)).astype(jnp.bfloat16)
        blocks = hidden.reshape(-1, N_TP, FE // N_TP).astype(jnp.float32)
        partials = jnp.einsum('rnf,nfd->nrd', blocks, weight_down.reshape(N_TP, FE // N_TP, D).astype(jnp.float32))
        partials = lax.optimization_barrier(partials.astype(jnp.bfloat16)).astype(jnp.float32)
        return lax.optimization_barrier(jnp.sum(partials, 0)).astype(jnp.bfloat16)
    expert_out = lax.map(expert, (slot_token, gate_w, up_w, down_w))
    source_row = jnp.arange(N_SP, dtype=jnp.int32)[:, None] * capacity
    pick_index = (flat_routes * (N_SP * capacity) + source_row + slot_rank).reshape(-1)
    picked = jnp.take(expert_out.reshape(-1, D), pick_index, axis=0).reshape(positions, 2, D)
    routed = lax.optimization_barrier(jnp.sum(picked.astype(jnp.float32) * route_weight[:, :, None], 1))
    return (stream_f + routed).astype(jnp.bfloat16)
```

```python
import jax
import jax.numpy as jnp
from jax import lax
from jax.experimental import pallas as pl
from jax.experimental.pallas import tpu as pltpu
from jax.sharding import Mesh
from jax.sharding import PartitionSpec as P

TP = ("tp_0", "tp_1")
epsilon = 1e-06
F32 = jnp.float32
BF16 = jnp.bfloat16
HALO = 32
EXTRA = 16


def in_vmem():
    return pl.BlockSpec(memory_space=pltpu.VMEM)


def call(kernel, outs, scratch=(), flops=0, name=None):
    return pl.pallas_call(
        kernel,
        out_shape=outs,
        out_specs=jax.tree.map(lambda _: in_vmem(), outs),
        scratch_shapes=list(scratch),
        name=name,
        cost_estimate=pl.CostEstimate(flops=flops, bytes_accessed=1 << 20, transcendentals=0),
        compiler_params=pltpu.CompilerParams(vmem_limit_bytes=48 * 2**20),
    )


def shape(dims, dtype=BF16):
    return jax.ShapeDtypeStruct(dims, dtype)


def down_lanes(row):
    return jnp.concatenate(
        [
            jnp.transpose(jnp.broadcast_to(row[:, i : i + 128], (128, 128)))
            for i in range(0, row.shape[1], 128)
        ],
        0,
    )


def gate_of(value, gate):
    return (value.astype(F32) * jax.nn.sigmoid(gate.astype(F32))).astype(BF16)


def tail_kernel(value, gate, docs, out):
    rows = value.shape[0]
    out[:HALO] = gate_of(value[rows - HALO :], gate[rows - HALO :])
    last = docs[docs.shape[0] - 1 :].astype(F32)
    out[HALO:] = down_lanes(last)[128 - HALO :].astype(BF16)


def conv_kernel(value, gate, docs, halo, taps, ln_gain, norm_gain, out, gext, dext):
    rows, chans = value.shape
    ntaps = taps.shape[0]
    gext[:HALO] = halo[:HALO].astype(F32)
    gext[HALO:] = gate_of(value[...], gate[...]).astype(F32)
    dext[:HALO] = halo[HALO:].astype(F32)
    for i in range(rows // 128):
        dext[HALO + 128 * i : HALO + 128 * (i + 1)] = down_lanes(docs[i : i + 1].astype(F32))
    kernel = taps[...].astype(F32)
    first = HALO - ntaps + 1
    step = 64
    means = []
    for r in range(0, rows, step):
        doc = dext[HALO + r : HALO + r + step]
        acc = jnp.zeros((step, chans), F32)
        for j in range(ntaps):
            at = first + j + r
            acc = acc + jnp.where(
                dext[at : at + step] == doc, gext[at : at + step] * kernel[j : j + 1], 0.0
            )
        mean = jnp.mean(acc, 1, keepdims=True)
        out[r : r + step] = (acc - mean).astype(BF16)
        means.append(jnp.broadcast_to(mean, (step, 128)))
    lines = []
    for i in range(rows // 128):
        lines.append(jnp.transpose(jnp.concatenate(means[2 * i : 2 * i + 2], 0))[:1])
    mean = jnp.concatenate(lines, 0)
    high = mean.astype(BF16).astype(F32)
    low = mean - high
    tail = jnp.concatenate(
        [high, low, ln_gain[...].astype(F32), norm_gain[...].astype(F32)], 0
    )
    tail = jnp.concatenate([tail, jnp.zeros((EXTRA - tail.shape[0], 128), F32)], 0)
    out[rows:] = tail.astype(BF16)


def routing_kernel(routes, weights, rank_out, pick_out, weight_out):
    rows = routes.shape[1]
    experts = rank_out.shape[0]
    capacity = 4 * rows // experts
    expert = lax.broadcasted_iota(jnp.int32, (experts, rows), 0)
    first = routes[:1] == expert
    second = routes[1:] == expert
    named = jnp.logical_or(first, second)
    before = lax.broadcasted_iota(jnp.int32, (rows, rows), 0) < lax.broadcasted_iota(
        jnp.int32, (rows, rows), 1
    )
    rank = jnp.dot(
        named.astype(F32).astype(BF16),
        before.astype(F32).astype(BF16),
        preferred_element_type=F32,
    )
    rank_out[...] = jnp.where(named, rank, -1.0)
    slot = rank + (expert * capacity).astype(F32)
    for k, chosen in enumerate((first, second)):
        pick = jnp.sum(jnp.where(chosen, slot, 0.0), 0, keepdims=True)
        pick_out[k] = down_lanes(pick)
        weight_out[k] = down_lanes(weights[k : k + 1])


def stream_kernel(parts, out_weight, residual, rank, stream_out, sent, means, full, act, place):
    peers, extended, chans = parts.shape
    rows = extended - EXTRA
    width = peers * chans
    for d in range(peers):
        tail = parts[d, rows:].astype(F32)
        for i in range(rows // 128):
            means[d : d + 1, 128 * i : 128 * (i + 1)] = tail[i : i + 1]
            means[peers + d : peers + d + 1, 128 * i : 128 * (i + 1)] = tail[
                rows // 128 + i : rows // 128 + i + 1
            ]
    owner = lax.broadcasted_iota(jnp.int32, (2 * peers, width), 0)
    block = lax.broadcasted_iota(jnp.int32, (2 * peers, width), 1) // chans
    spread = jnp.logical_or(owner == block, owner == block + peers).astype(F32).astype(BF16)
    full[...] = lax.dot_general(
        means[...].astype(BF16),
        spread,
        (((0,), (0,)), ((), ())),
        preferred_element_type=F32,
    )
    nextra = 2 * (rows // 128)
    step = 64
    for r in range(0, rows, step):
        total = jnp.zeros((step, chans), F32)
        square = jnp.zeros((step, chans), F32)
        for d in range(peers):
            x = full[r : r + step, d * chans : (d + 1) * chans] + parts[d, r : r + step].astype(F32)
            full[r : r + step, d * chans : (d + 1) * chans] = x
            total = total + x
            square = square + x * x
        mean = jnp.sum(total, 1, keepdims=True) / width
        var = jnp.sum(square, 1, keepdims=True) / width - mean * mean
        scale = lax.rsqrt(var + epsilon)
        for d in range(peers):
            gain = parts[d, rows:].astype(F32)[nextra : nextra + 1]
            x = full[r : r + step, d * chans : (d + 1) * chans]
            x = (x - mean) * scale * gain
            act[r : r + step, d * chans : (d + 1) * chans] = (x / (1.0 + jnp.exp(-x))).astype(BF16)
    projected = jnp.dot(act[...], out_weight[...], preferred_element_type=F32).astype(BF16)
    stream = (residual[...].astype(F32) + projected.astype(F32)).astype(BF16)
    stream_out[...] = stream
    experts, capacity, _ = sent.shape
    slot = lax.broadcasted_iota(jnp.int32, (capacity, rows), 0).astype(F32)
    for e in range(experts):
        place[e * capacity : (e + 1) * capacity] = (
            (rank[e : e + 1] == slot).astype(F32).astype(BF16)
        )
    moved = jnp.dot(place[...], stream, preferred_element_type=F32).astype(BF16)
    sent[...] = moved.reshape(sent.shape)


def expert_kernel(parts, gains, gate_a, up_a, down_a, gate_b, up_b, down_b, out, normed):
    peers, rows, chans = parts.shape
    width = peers * chans
    step = 64
    for r in range(0, rows, step):
        square = jnp.zeros((step, chans), F32)
        for d in range(peers):
            x = parts[d, r : r + step].astype(F32)
            square = square + x * x
        scale = lax.rsqrt(jnp.sum(square, 1, keepdims=True) / width + epsilon)
        for d in range(peers):
            x = parts[d, r : r + step].astype(F32) * scale * gains[d : d + 1].astype(F32)
            normed[r : r + step, d * chans : (d + 1) * chans] = x.astype(BF16)
    step = 256
    for r in range(0, rows, step):
        x = normed[r : r + step]
        hidden = []
        for gate_w, up_w in ((gate_a, up_a), (gate_b, up_b)):
            gate = jnp.dot(x, gate_w[...], preferred_element_type=F32)
            up = jnp.dot(x, up_w[...], preferred_element_type=F32)
            hidden.append((gate / (1.0 + jnp.exp(-gate)) * up).astype(BF16))
        for c in range(0, width, 512):
            y = jnp.dot(hidden[0], down_a[:, c : c + 512], preferred_element_type=F32)
            y = y + jnp.dot(hidden[1], down_b[:, c : c + 512], preferred_element_type=F32)
            y = y.astype(BF16)
            for i in range(512 // chans):
                out[c // chans + i, r : r + step] = y[:, i * chans : (i + 1) * chans]


def mix_kernel(returned, pick, weight, stream, out):
    rows = stream.shape[0]
    slots = returned.shape[0]
    lane = lax.broadcasted_iota(jnp.int32, (rows, 128), 1).astype(F32)
    routed = jnp.zeros(stream.shape, F32)
    back = returned[...]
    for k in range(2):
        choose = jnp.concatenate(
            [
                (pick[k] == lane + float(s)).astype(F32).astype(BF16)
                for s in range(0, slots, 128)
            ],
            1,
        )
        picked = jnp.dot(choose, back, preferred_element_type=F32)
        routed = routed + picked * weight[k]
    out[...] = (stream[...].astype(F32) + routed).astype(BF16)


def to_each(x, axis):
    copies = jnp.broadcast_to(x, (lax.axis_size(axis), *x.shape))
    return lax.all_to_all(copies, axis, split_axis=0, concat_axis=0, tiled=True)


def swap_pair(x):
    peers = lax.axis_size("tp_1")
    return lax.ppermute(x, "tp_1", [(i, i ^ 1) for i in range(peers)])


def per_device(
    residual_in,
    conv_value,
    conv_gate,
    doc_ids,
    conv_kernel_w,
    ln_gain,
    out_weight,
    norm_gain,
    routes,
    route_weight,
    gate_w,
    up_w,
    down_w,
):
    rows, chans = conv_value.shape
    experts = lax.axis_size("sp")
    peers = lax.axis_size(TP)
    capacity = 4 * rows // experts
    slots = experts * capacity
    width = peers * chans
    docs = doc_ids.reshape(rows // 128, 128)
    gate_a, up_a, down_a = gate_w[0], up_w[0], down_w[0]

    tail = call(tail_kernel, shape((2 * HALO, chans)), name="tail")(conv_value, conv_gate, docs)
    n = lax.axis_size("sp")
    halo = lax.ppermute(tail, "sp", [(i, i + 1) for i in range(n - 1)])
    gate_b, up_b, down_b = swap_pair(gate_a), swap_pair(up_a), swap_pair(down_a)
    packed = call(
        conv_kernel,
        shape((rows + EXTRA, chans)),
        [pltpu.VMEM((rows + HALO, chans), F32), pltpu.VMEM((rows + HALO, chans), F32)],
        name="conv",
    )(
        conv_value,
        conv_gate,
        docs,
        halo,
        conv_kernel_w,
        ln_gain.reshape(1, chans),
        norm_gain.reshape(1, chans),
    )
    rank, pick, weight = call(
        routing_kernel,
        (shape((experts, rows), F32), shape((2, rows, 128), F32), shape((2, rows, 128), F32)),
        name="routing",
    )(routes.T, route_weight.T)
    parts = to_each(packed, TP)
    stream, sent = call(
        stream_kernel,
        (shape((rows, chans)), shape((experts, capacity, chans))),
        [
            pltpu.VMEM((2 * peers, rows), F32),
            pltpu.VMEM((rows, width), F32),
            pltpu.VMEM((rows, width), BF16),
            pltpu.VMEM((slots, rows), BF16),
        ],
        name="stream",
    )(parts, out_weight, residual_in, rank)
    gains = parts[:, rows + 2 * (rows // 128) + 1, :]
    received = lax.all_to_all(sent, "sp", split_axis=0, concat_axis=0, tiled=True)
    half = slots // 2
    outbound = jnp.broadcast_to(
        received.reshape(1, 2, half, chans), (peers // 2, 2, half, chans)
    ).reshape(peers, half, chans)
    gathered = lax.all_to_all(outbound, TP, split_axis=0, concat_axis=0, tiled=True)
    partial = call(
        expert_kernel,
        shape((peers, half, chans)),
        [pltpu.VMEM((half, width), BF16)],
        name="expert",
    )(gathered, gains, gate_a, up_a, down_a, gate_b, up_b, down_b)
    pieces = lax.all_to_all(partial, TP, split_axis=0, concat_axis=0, tiled=True)
    summed = jnp.sum(pieces.reshape(peers // 2, 2, half, chans).astype(F32), 0).astype(BF16)
    returned = lax.all_to_all(
        summed.reshape(experts, capacity, chans), "sp", split_axis=0, concat_axis=0, tiled=True
    )
    return call(mix_kernel, shape((rows, chans)), name="mix")(
        returned.reshape(slots, chans), pick, weight, stream
    )


def solution(mesh):
    split = Mesh(mesh.devices.reshape(mesh.shape["sp"], 4, 4), ("sp", "tp_0", "tp_1"))
    in_specs = (
        P("sp", TP),
        P("sp", TP),
        P("sp", TP),
        P("sp"),
        P(None, TP),
        P(TP),
        P(None, TP),
        P(TP),
        P("sp", None),
        P("sp", None),
        P("sp", None, TP),
        P("sp", None, TP),
        P("sp", TP, None),
    )
    out_specs = P("sp", TP)
    return jax.shard_map(
        per_device, mesh=split, in_specs=in_specs, out_specs=out_specs, check_vma=False
    )
```

```python
import jax
import jax.numpy as jnp
from jax import lax
from jax.experimental import pallas as pl
from jax.experimental.pallas import tpu as pltpu
from jax.sharding import Mesh
from jax.sharding import PartitionSpec as P


TP = ("tp_0", "tp_1")
epsilon = 1e-06
F32 = jnp.float32
BF16 = jnp.bfloat16
HALO = 32
EXTRA = 16


def vmem(dims, dtype=BF16):
    return pltpu.VMEM(dims, dtype)


def call(kernel, outs, ins, scratch=(), copies=0, spread=False, flops=0):
    space = {"h": pltpu.HBM, "v": pltpu.VMEM}
    sems = [pltpu.SemaphoreType.DMA((copies,))] if copies else []
    out_space = pltpu.HBM if spread else pltpu.VMEM
    return pl.pallas_call(
        kernel,
        out_shape=outs,
        in_specs=[pl.BlockSpec(memory_space=space[c]) for c in ins],
        out_specs=jax.tree.map(lambda _: pl.BlockSpec(memory_space=out_space), outs),
        scratch_shapes=list(scratch) + sems,
        cost_estimate=pl.CostEstimate(flops=flops, bytes_accessed=1 << 20, transcendentals=0),
        compiler_params=pltpu.CompilerParams(vmem_limit_bytes=48 * 2**20),
    )


def start(pairs, sems, first=0):
    made = [
        pltpu.make_async_copy(src, dst, sems.at[first + i]) for i, (src, dst) in enumerate(pairs)
    ]
    for copy in made:
        copy.start()
    return made


def finish(made):
    for copy in made:
        copy.wait()


def half_of(core, peer):
    return jnp.where(core == 0, peer % 2, (peer // 4) % 2)


def shape(dims, dtype=BF16):
    return jax.ShapeDtypeStruct(dims, dtype)


def down_lanes(row):
    return jnp.concatenate(
        [
            jnp.transpose(jnp.broadcast_to(row[:, i : i + 128], (128, 128)))
            for i in range(0, row.shape[1], 128)
        ],
        0,
    )


def gate_of(value, gate):
    return (value.astype(F32) * jax.nn.sigmoid(gate.astype(F32))).astype(BF16)


def tail_kernel(value_h, gate_h, docs_h, out, value, gate, docs, sems):
    rows = value_h.shape[0]
    finish(
        start(
            [
                (value_h.at[rows - HALO :], value),
                (gate_h.at[rows - HALO :], gate),
                (docs_h, docs),
            ],
            sems,
        )
    )
    out[:HALO] = gate_of(value[...], gate[...])
    last = docs[docs.shape[0] - 1 :].astype(F32)
    out[HALO:] = down_lanes(last)[128 - HALO :].astype(BF16)


def conv_kernel(
    halo,
    value_h,
    gate_h,
    docs_h,
    taps_h,
    ln_gain_h,
    norm_gain_h,
    sent,
    value,
    gate,
    docs,
    taps,
    ln_gain,
    norm_gain,
    gext,
    dext,
    out,
    sems,
):
    finish(
        start(
            [
                (value_h, value),
                (gate_h, gate),
                (docs_h, docs),
                (taps_h, taps),
                (ln_gain_h, ln_gain),
                (norm_gain_h, norm_gain),
            ],
            sems,
        )
    )
    rows, chans = value.shape
    ntaps = taps.shape[0]
    gext[:HALO] = halo[:HALO].astype(F32)
    gext[HALO:] = gate_of(value[...], gate[...]).astype(F32)
    dext[:HALO] = halo[HALO:].astype(F32)
    for i in range(rows // 128):
        dext[HALO + 128 * i : HALO + 128 * (i + 1)] = down_lanes(docs[i : i + 1].astype(F32))
    kernel = taps[...].astype(F32)
    first = HALO - ntaps + 1
    step = 64
    means = []
    for r in range(0, rows, step):
        doc = dext[HALO + r : HALO + r + step]
        acc = jnp.zeros((step, chans), F32)
        for j in range(ntaps):
            at = first + j + r
            acc = acc + jnp.where(
                dext[at : at + step] == doc, gext[at : at + step] * kernel[j : j + 1], 0.0
            )
        mean = jnp.mean(acc, 1, keepdims=True)
        out[r : r + step] = (acc - mean).astype(BF16)
        means.append(jnp.broadcast_to(mean, (step, 128)))
    lines = []
    for i in range(rows // 128):
        lines.append(jnp.transpose(jnp.concatenate(means[2 * i : 2 * i + 2], 0))[:1])
    mean = jnp.concatenate(lines, 0)
    high = mean.astype(BF16).astype(F32)
    low = mean - high
    tail = jnp.concatenate(
        [high, low, ln_gain[...].astype(F32), norm_gain[...].astype(F32)], 0
    )
    tail = jnp.concatenate([tail, jnp.zeros((EXTRA - tail.shape[0], 128), F32)], 0)
    out[rows:] = tail.astype(BF16)
    finish(start([(out, sent.at[i]) for i in range(sent.shape[0])], sems))


def routing_kernel(routes, weights, rank_out, pick_out, weight_out):
    rows = routes.shape[1]
    experts = rank_out.shape[0]
    capacity = 4 * rows // experts
    expert = lax.broadcasted_iota(jnp.int32, (experts, rows), 0)
    first = routes[:1] == expert
    second = routes[1:] == expert
    named = jnp.logical_or(first, second)
    before = lax.broadcasted_iota(jnp.int32, (rows, rows), 0) < lax.broadcasted_iota(
        jnp.int32, (rows, rows), 1
    )
    rank = jnp.dot(
        named.astype(F32).astype(BF16),
        before.astype(F32).astype(BF16),
        preferred_element_type=F32,
    )
    rank_out[...] = jnp.where(named, rank, -1.0)
    slot = rank + (expert * capacity).astype(F32)
    for k, chosen in enumerate((first, second)):
        pick = jnp.sum(jnp.where(chosen, slot, 0.0), 0, keepdims=True)
        pick_out[k] = down_lanes(pick)
        weight_out[k] = down_lanes(weights[k : k + 1])


def stream_kernel(parts, out_weight, residual, rank, stream_out, sent, means, full, act, place):
    peers, extended, chans = parts.shape
    rows = extended - EXTRA
    width = peers * chans
    for d in range(peers):
        tail = parts[d, rows:].astype(F32)
        for i in range(rows // 128):
            means[d : d + 1, 128 * i : 128 * (i + 1)] = tail[i : i + 1]
            means[peers + d : peers + d + 1, 128 * i : 128 * (i + 1)] = tail[
                rows // 128 + i : rows // 128 + i + 1
            ]
    owner = lax.broadcasted_iota(jnp.int32, (2 * peers, width), 0)
    block = lax.broadcasted_iota(jnp.int32, (2 * peers, width), 1) // chans
    spread = jnp.logical_or(owner == block, owner == block + peers).astype(F32).astype(BF16)
    full[...] = lax.dot_general(
        means[...].astype(BF16),
        spread,
        (((0,), (0,)), ((), ())),
        preferred_element_type=F32,
    )
    nextra = 2 * (rows // 128)
    step = 64
    for r in range(0, rows, step):
        total = jnp.zeros((step, chans), F32)
        square = jnp.zeros((step, chans), F32)
        for d in range(peers):
            x = full[r : r + step, d * chans : (d + 1) * chans] + parts[d, r : r + step].astype(F32)
            full[r : r + step, d * chans : (d + 1) * chans] = x
            total = total + x
            square = square + x * x
        mean = jnp.sum(total, 1, keepdims=True) / width
        var = jnp.sum(square, 1, keepdims=True) / width - mean * mean
        scale = lax.rsqrt(var + epsilon)
        for d in range(peers):
            gain = parts[d, rows:].astype(F32)[nextra : nextra + 1]
            x = full[r : r + step, d * chans : (d + 1) * chans]
            x = (x - mean) * scale * gain
            act[r : r + step, d * chans : (d + 1) * chans] = (x / (1.0 + jnp.exp(-x))).astype(BF16)
    projected = jnp.dot(act[...], out_weight[...], preferred_element_type=F32).astype(BF16)
    stream = (residual[...].astype(F32) + projected.astype(F32)).astype(BF16)
    stream_out[...] = stream
    experts, capacity, _ = sent.shape
    slot = lax.broadcasted_iota(jnp.int32, (capacity, rows), 0).astype(F32)
    for e in range(experts):
        place[e * capacity : (e + 1) * capacity] = (
            (rank[e : e + 1] == slot).astype(F32).astype(BF16)
        )
    moved = jnp.dot(place[...], stream, preferred_element_type=F32).astype(BF16)
    sent[...] = moved.reshape(sent.shape)


def spread_kernel(received, out, sems):
    core = lax.axis_index("sp") % 2
    peers, half, _ = out.shape
    pairs = []
    for i in range(peers):
        first = pl.multiple_of(half_of(core, i) * half, half)
        pairs.append((received.at[pl.ds(first, half)], out.at[i]))
    finish(start(pairs, sems))


def expert_kernel(
    parts,
    gains,
    gate_ah,
    up_ah,
    down_ah,
    gate_bh,
    up_bh,
    down_bh,
    out,
    normed,
    gate_a,
    up_a,
    down_a,
    gate_b,
    up_b,
    down_b,
    sems,
):
    made = start(
        [
            (gate_ah, gate_a),
            (up_ah, up_a),
            (gate_bh, gate_b),
            (up_bh, up_b),
            (down_ah, down_a),
            (down_bh, down_b),
        ],
        sems,
    )
    peers, rows, chans = parts.shape
    width = peers * chans
    step = 64
    for r in range(0, rows, step):
        square = jnp.zeros((step, chans), F32)
        for d in range(peers):
            x = parts[d, r : r + step].astype(F32)
            square = square + x * x
        scale = lax.rsqrt(jnp.sum(square, 1, keepdims=True) / width + epsilon)
        for d in range(peers):
            x = parts[d, r : r + step].astype(F32) * scale * gains[d : d + 1].astype(F32)
            normed[r : r + step, d * chans : (d + 1) * chans] = x.astype(BF16)
    finish(made)
    step = 256
    for r in range(0, rows, step):
        x = normed[r : r + step]
        hidden = []
        for gate_w, up_w in ((gate_a, up_a), (gate_b, up_b)):
            gate = jnp.dot(x, gate_w[...], preferred_element_type=F32)
            up = jnp.dot(x, up_w[...], preferred_element_type=F32)
            hidden.append((gate / (1.0 + jnp.exp(-gate)) * up).astype(BF16))
        for c in range(0, width, 512):
            y = jnp.dot(hidden[0], down_a[:, c : c + 512], preferred_element_type=F32)
            y = y + jnp.dot(hidden[1], down_b[:, c : c + 512], preferred_element_type=F32)
            y = y.astype(BF16)
            for i in range(512 // chans):
                out[c // chans + i, r : r + step] = y[:, i * chans : (i + 1) * chans]


def sum_kernel(pieces, out):
    core = lax.axis_index("sp") % 2
    peers, half, _ = pieces.shape
    for h in range(2):
        total = jnp.zeros(pieces.shape[1:], F32)
        for k in range(peers // 2):
            across = (k // 2) * 4 + (k % 2) * 2 + h
            down = ((k // 4) * 2 + h) * 4 + k % 4
            total = total + pieces[jnp.where(core == 0, across, down)].astype(F32)
        out[h * half : (h + 1) * half] = total.astype(BF16)


def mix_kernel(returned, pick, weight, stream, out):
    rows = stream.shape[0]
    slots = returned.shape[0]
    lane = lax.broadcasted_iota(jnp.int32, (rows, 128), 1).astype(F32)
    routed = jnp.zeros(stream.shape, F32)
    back = returned[...]
    for k in range(2):
        choose = jnp.concatenate(
            [
                (pick[k] == lane + float(s)).astype(F32).astype(BF16)
                for s in range(0, slots, 128)
            ],
            1,
        )
        picked = jnp.dot(choose, back, preferred_element_type=F32)
        routed = routed + picked * weight[k]
    out[...] = (stream[...].astype(F32) + routed).astype(BF16)


def exchange(x, axis):
    return lax.all_to_all(x, axis, split_axis=0, concat_axis=0, tiled=True)


def swap_pair(x):
    groups, peers = lax.axis_size("sp"), lax.axis_size(TP)
    pairs = [
        (s * peers + t, s * peers + (t ^ (1 if s % 2 == 0 else 4)))
        for s in range(groups)
        for t in range(peers)
    ]
    return lax.ppermute(x, ("sp", *TP), pairs)


def per_device(
    residual_in,
    conv_value,
    conv_gate,
    doc_ids,
    conv_kernel_w,
    ln_gain,
    out_weight,
    norm_gain,
    routes,
    route_weight,
    gate_w,
    up_w,
    down_w,
):
    rows, chans = conv_value.shape
    experts = lax.axis_size("sp")
    peers = lax.axis_size(TP)
    capacity = 4 * rows // experts
    slots = experts * capacity
    width = peers * chans
    docs = doc_ids.reshape(rows // 128, 128)
    gate_a, up_a, down_a = gate_w[0], up_w[0], down_w[0]

    tail = call(
        tail_kernel,
        shape((2 * HALO, chans)),
        "hhh",
        [vmem((HALO, chans)), vmem((HALO, chans)), vmem(docs.shape, jnp.int32)],
        copies=3,
    )(conv_value, conv_gate, docs)
    n = lax.axis_size("sp")
    halo = lax.ppermute(tail, "sp", [(i, i + 1) for i in range(n - 1)])
    gate_b = swap_pair(gate_a)
    up_b = swap_pair(up_a)
    down_b = swap_pair(down_a)
    packed = call(
        conv_kernel,
        shape((peers, rows + EXTRA, chans)),
        "vhhhhhh",
        [
            vmem((rows, chans)),
            vmem((rows, chans)),
            vmem(docs.shape, jnp.int32),
            vmem(conv_kernel_w.shape),
            vmem((1, chans)),
            vmem((1, chans)),
            vmem((rows + HALO, chans), F32),
            vmem((rows + HALO, chans), F32),
            vmem((rows + EXTRA, chans)),
        ],
        copies=peers,
        spread=True,
    )(
        halo,
        conv_value,
        conv_gate,
        docs,
        conv_kernel_w,
        ln_gain.reshape(1, chans),
        norm_gain.reshape(1, chans),
    )
    rank, pick, weight = call(
        routing_kernel,
        (shape((experts, rows), F32), shape((2, rows, 128), F32), shape((2, rows, 128), F32)),
        "vv",
    )(routes.T, route_weight.T)
    parts = exchange(packed, TP)
    stream, sent = call(
        stream_kernel,
        (shape((rows, chans)), shape((experts, capacity, chans))),
        "vvvv",
        [
            vmem((2 * peers, rows), F32),
            vmem((rows, width), F32),
            vmem((rows, width)),
            vmem((slots, rows)),
        ],
    )(parts, out_weight, residual_in, rank)
    gains = parts[:, rows + 2 * (rows // 128) + 1, :]
    received = exchange(sent, "sp")
    half = slots // 2
    outbound = call(
        spread_kernel, shape((peers, half, chans)), "v", copies=peers, spread=True
    )(received.reshape(slots, chans))
    gathered = exchange(outbound, TP)
    partial = call(
        expert_kernel,
        shape((peers, half, chans)),
        "vvhhhhhh",
        [vmem((half, width))]
        + [vmem(gate_a.shape), vmem(up_a.shape), vmem(down_a.shape)] * 2,
        copies=6,
    )(gathered, gains, gate_a, up_a, down_a, gate_b, up_b, down_b)
    pieces = exchange(partial, TP)
    summed = call(sum_kernel, shape((slots, chans)), "v")(pieces)
    returned = exchange(summed.reshape(experts, capacity, chans), "sp")
    return call(mix_kernel, shape((rows, chans)), "vvvv")(
        returned.reshape(slots, chans), pick, weight, stream
    )


def solution(mesh):
    split = Mesh(mesh.devices.reshape(mesh.shape["sp"], 4, 4), ("sp", "tp_0", "tp_1"))
    in_specs = (
        P("sp", TP),
        P("sp", TP),
        P("sp", TP),
        P("sp"),
        P(None, TP),
        P(TP),
        P(None, TP),
        P(TP),
        P("sp", None),
        P("sp", None),
        P("sp", None, TP),
        P("sp", None, TP),
        P("sp", TP, None),
    )
    out_specs = P("sp", TP)
    return jax.shard_map(
        per_device, mesh=split, in_specs=in_specs, out_specs=out_specs, check_vma=False
    )
```

```python
import jax
import jax.numpy as jnp
from jax import lax
from jax.experimental import pallas as pl
from jax.experimental.pallas import tpu as pltpu
from jax.sharding import Mesh
from jax.sharding import PartitionSpec as P


TP = ("tp_0", "tp_1")
epsilon = 1e-06
F32 = jnp.float32
BF16 = jnp.bfloat16
HALO = 32
CHUNKS = 1
EXTRA = 16


def vmem(dims, dtype=BF16):
    return pltpu.VMEM(dims, dtype)


def call(kernel, outs, ins, scratch=(), copies=0, spread=False, mib=4, flops=0):
    space = {"h": pltpu.HBM, "v": pltpu.VMEM}
    sems = [pltpu.SemaphoreType.DMA((copies,))] if copies else []
    out_space = pltpu.HBM if spread else pltpu.VMEM
    return pl.pallas_call(
        kernel,
        out_shape=outs,
        in_specs=[pl.BlockSpec(memory_space=space[c]) for c in ins],
        out_specs=jax.tree.map(lambda _: pl.BlockSpec(memory_space=out_space), outs),
        scratch_shapes=list(scratch) + sems,
        cost_estimate=pl.CostEstimate(flops=flops, bytes_accessed=0, transcendentals=0),
        compiler_params=pltpu.CompilerParams(vmem_limit_bytes=mib * 2**20),
    )


def start(pairs, sems, first=0):
    made = [
        pltpu.make_async_copy(src, dst, sems.at[first + i]) for i, (src, dst) in enumerate(pairs)
    ]
    for copy in made:
        copy.start()
    return made


def finish(made):
    for copy in made:
        copy.wait()


def place_of(core, peer):
    return jnp.where(core == 0, peer, (peer % 4) * 4 + peer // 4)


def shape(dims, dtype=BF16):
    return jax.ShapeDtypeStruct(dims, dtype)


def down_lanes(row):
    return jnp.concatenate(
        [
            jnp.transpose(jnp.broadcast_to(row[:, i : i + 128], (128, 128)))
            for i in range(0, row.shape[1], 128)
        ],
        0,
    )


def gate_of(value, gate):
    return (value.astype(F32) * jax.nn.sigmoid(gate.astype(F32))).astype(BF16)


def conv_kernel(halo, gated, docs, consts, sent, gext, dext, out, sems):
    rows, chans = gated.shape
    ntaps = consts.shape[0] - 2
    gext[:HALO] = halo[:HALO].astype(F32)
    gext[HALO:] = gated[...].astype(F32)
    dext[:HALO] = halo[HALO:].astype(F32)
    dext[HALO:] = docs[...].astype(F32)
    kernel = consts[...].astype(F32)
    first = HALO - ntaps + 1
    step = 64
    means = []
    for r in range(0, rows, step):
        doc = dext[HALO + r : HALO + r + step]
        acc = jnp.zeros((step, chans), F32)
        for j in range(ntaps):
            at = first + j + r
            acc = acc + jnp.where(
                dext[at : at + step] == doc, gext[at : at + step] * kernel[j : j + 1], 0.0
            )
        mean = jnp.mean(acc, 1, keepdims=True)
        out[r : r + step] = (acc - mean).astype(BF16)
        means.append(jnp.broadcast_to(mean, (step, 128)))
    lines = []
    for i in range(rows // 128):
        lines.append(jnp.transpose(jnp.concatenate(means[2 * i : 2 * i + 2], 0))[:1])
    mean = jnp.concatenate(lines, 0)
    high = mean.astype(BF16).astype(F32)
    low = mean - high
    tail = jnp.concatenate([high, low, kernel[ntaps:]], 0)
    tail = jnp.concatenate([tail, jnp.zeros((EXTRA - tail.shape[0], 128), F32)], 0)
    out[rows:] = tail.astype(BF16)
    finish(start([(out, sent.at[i]) for i in range(sent.shape[0])], sems))


def routing_kernel(routes, weights, rank_out, pick_out, weight_out):
    rows = routes.shape[1]
    experts = rank_out.shape[0]
    part = 4 * rows // experts // CHUNKS
    expert = lax.broadcasted_iota(jnp.int32, (experts, rows), 0)
    first = routes[:1] == expert
    second = routes[1:] == expert
    named = jnp.logical_or(first, second)
    before = lax.broadcasted_iota(jnp.int32, (rows, rows), 0) < lax.broadcasted_iota(
        jnp.int32, (rows, rows), 1
    )
    rank = jnp.dot(
        named.astype(F32).astype(BF16),
        before.astype(F32).astype(BF16),
        preferred_element_type=F32,
    )
    rank_out[...] = jnp.where(named, rank, -1.0)
    slot = rank + (expert * part).astype(F32)
    for c in range(1, CHUNKS):
        slot = slot + jnp.where(rank >= c * part, float((experts - 1) * part), 0.0)
    for k, chosen in enumerate((first, second)):
        pick = jnp.sum(jnp.where(chosen, slot, 0.0), 0, keepdims=True)
        pick_out[k] = down_lanes(pick)
        weight_out[k] = down_lanes(weights[k : k + 1])


def stream_kernel(parts, out_weight, residual, rank, stream_out, gains, *rest):
    core = lax.axis_index("sp") % 2
    sent, (means, full, act, place) = rest[:CHUNKS], rest[CHUNKS:]
    peers, extended, chans = parts.shape
    rows = extended - EXTRA
    width = peers * chans
    for d in range(peers):
        tail = parts[place_of(core, d), rows:].astype(F32)
        gains[d : d + 1] = tail[2 * (rows // 128) + 1 : 2 * (rows // 128) + 2]
        for i in range(rows // 128):
            means[d : d + 1, 128 * i : 128 * (i + 1)] = tail[i : i + 1]
            means[peers + d : peers + d + 1, 128 * i : 128 * (i + 1)] = tail[
                rows // 128 + i : rows // 128 + i + 1
            ]
    owner = lax.broadcasted_iota(jnp.int32, (2 * peers, width), 0)
    block = lax.broadcasted_iota(jnp.int32, (2 * peers, width), 1) // chans
    spread = jnp.logical_or(owner == block, owner == block + peers).astype(F32).astype(BF16)
    full[...] = lax.dot_general(
        means[...].astype(BF16),
        spread,
        (((0,), (0,)), ((), ())),
        preferred_element_type=F32,
    )
    nextra = 2 * (rows // 128)
    step = 64
    for r in range(0, rows, step):
        total = jnp.zeros((step, chans), F32)
        square = jnp.zeros((step, chans), F32)
        for d in range(peers):
            x = full[r : r + step, d * chans : (d + 1) * chans] + parts[
                place_of(core, d), r : r + step
            ].astype(F32)
            full[r : r + step, d * chans : (d + 1) * chans] = x
            total = total + x
            square = square + x * x
        mean = jnp.sum(total, 1, keepdims=True) / width
        var = jnp.sum(square, 1, keepdims=True) / width - mean * mean
        scale = lax.rsqrt(var + epsilon)
        for d in range(peers):
            gain = parts[place_of(core, d), rows:].astype(F32)[nextra : nextra + 1]
            x = full[r : r + step, d * chans : (d + 1) * chans]
            x = (x - mean) * scale * gain
            act[r : r + step, d * chans : (d + 1) * chans] = (x / (1.0 + jnp.exp(-x))).astype(BF16)
    projected = jnp.dot(act[...], out_weight[...], preferred_element_type=F32).astype(BF16)
    stream = (residual[...].astype(F32) + projected.astype(F32)).astype(BF16)
    stream_out[...] = stream
    experts, part, _ = sent[0].shape
    slots = experts * part
    slot = lax.broadcasted_iota(jnp.int32, (part, rows), 0)
    for c in range(CHUNKS):
        wanted = (slot + c * part).astype(F32)
        for e in range(experts):
            at = c * slots + e * part
            place[at : at + part] = (rank[e : e + 1] == wanted).astype(F32).astype(BF16)
    moved = jnp.dot(place[...], stream, preferred_element_type=F32).astype(BF16)
    for c in range(CHUNKS):
        sent[c][...] = moved[c * slots : (c + 1) * slots].reshape(sent[c].shape)


def expert_kernel(
    parts,
    gains,
    gate_ah,
    up_ah,
    down_ah,
    gate_bh,
    up_bh,
    down_bh,
    out,
    normed,
    gate_a,
    up_a,
    down_a,
    gate_b,
    up_b,
    down_b,
    sems,
):
    made = start(
        [
            (gate_ah, gate_a),
            (up_ah, up_a),
            (gate_bh, gate_b),
            (up_bh, up_b),
            (down_ah, down_a),
            (down_bh, down_b),
        ],
        sems,
    )
    core = lax.axis_index("sp") % 2
    peers, rows, chans = parts.shape
    width = peers * chans
    step = 64
    for r in range(0, rows, step):
        square = jnp.zeros((step, chans), F32)
        for d in range(peers):
            x = parts[d, r : r + step].astype(F32)
            square = square + x * x
        scale = lax.rsqrt(jnp.sum(square, 1, keepdims=True) / width + epsilon)
        for d in range(peers):
            x = parts[place_of(core, d), r : r + step].astype(F32) * scale * gains[d : d + 1]
            normed[r : r + step, d * chans : (d + 1) * chans] = x.astype(BF16)
    finish(made)
    step = 256
    for r in range(0, rows, step):
        x = normed[r : r + step]
        hidden = []
        for gate_w, up_w in ((gate_a, up_a), (gate_b, up_b)):
            gate = jnp.dot(x, gate_w[...], preferred_element_type=F32)
            up = jnp.dot(x, up_w[...], preferred_element_type=F32)
            hidden.append((gate / (1.0 + jnp.exp(-gate)) * up).astype(BF16))
        for c in range(0, width, 512):
            y = jnp.dot(hidden[0], down_a[:, c : c + 512], preferred_element_type=F32)
            y = y + jnp.dot(hidden[1], down_b[:, c : c + 512], preferred_element_type=F32)
            y = y.astype(BF16)
            for i in range(512 // chans):
                out[place_of(core, c // chans + i), r : r + step] = y[:, i * chans : (i + 1) * chans]


def mix_kernel(*refs):
    returned, (pick, weight, stream, out) = refs[:CHUNKS], refs[CHUNKS:]
    rows = stream.shape[0]
    slots = returned[0].shape[0]
    lane = lax.broadcasted_iota(jnp.int32, (rows, 128), 1).astype(F32)
    routed = jnp.zeros(stream.shape, F32)
    for k in range(2):
        picked = jnp.zeros(stream.shape, F32)
        for c in range(CHUNKS):
            choose = jnp.concatenate(
                [
                    (pick[k] == lane + float(c * slots + s)).astype(F32).astype(BF16)
                    for s in range(0, slots, 128)
                ],
                1,
            )
            picked = picked + jnp.dot(choose, returned[c][...], preferred_element_type=F32)
        routed = routed + picked * weight[k]
    out[...] = (stream[...].astype(F32) + routed).astype(BF16)


def exchange(x, axis):
    return lax.all_to_all(x, axis, split_axis=0, concat_axis=0, tiled=True)


def rings(first):
    groups = []
    for s in range(lax.axis_size("sp")):
        along_x = (s % 2 == 0) == first
        for a in range(4):
            groups.append([s * 16 + (4 * a + b if along_x else 4 * b + a) for b in range(4)])
    return groups


def ring_exchange(x, first):
    return lax.all_to_all(
        x, ("sp", *TP), split_axis=0, concat_axis=0, axis_index_groups=rings(first), tiled=True
    )


def four_copies(x):
    return jnp.broadcast_to(x, (4, *x.shape))


def swap_pair(x):
    groups, peers = lax.axis_size("sp"), lax.axis_size(TP)
    pairs = [
        (s * peers + t, s * peers + (t ^ (1 if s % 2 == 0 else 4)))
        for s in range(groups)
        for t in range(peers)
    ]
    return lax.ppermute(x, ("sp", *TP), pairs)


def per_device(
    residual_in,
    conv_value,
    conv_gate,
    doc_ids,
    conv_kernel_w,
    ln_gain,
    out_weight,
    norm_gain,
    routes,
    route_weight,
    gate_w,
    up_w,
    down_w,
):
    rows, chans = conv_value.shape
    experts = lax.axis_size("sp")
    peers = lax.axis_size(TP)
    capacity = 4 * rows // experts
    slots = experts * capacity
    width = peers * chans
    gate_a, up_a, down_a = gate_w[0], up_w[0], down_w[0]

    gated = gate_of(conv_value, conv_gate)
    docs = jnp.broadcast_to(doc_ids.astype(BF16)[:, None], (rows, chans))
    consts = jnp.concatenate([conv_kernel_w, ln_gain[None], norm_gain[None]], 0)
    tail = jnp.concatenate(
        [
            gate_of(conv_value[rows - HALO :], conv_gate[rows - HALO :]),
            jnp.broadcast_to(doc_ids[rows - HALO :].astype(BF16)[:, None], (HALO, chans)),
        ],
        0,
    )
    n = lax.axis_size("sp")
    halo = lax.ppermute(tail, "sp", [(i, i + 1) for i in range(n - 1)])
    gate_b = swap_pair(gate_a)
    up_b = swap_pair(up_a)
    down_b = swap_pair(down_a)
    packed = call(
        conv_kernel,
        shape((4, rows + EXTRA, chans)),
        "vvvv",
        [
            vmem((rows + HALO, chans), F32),
            vmem((rows + HALO, chans), F32),
            vmem((rows + EXTRA, chans)),
        ],
        copies=4,
        spread=True,
    )(halo, gated, docs, consts)
    rank, pick, weight = call(
        routing_kernel,
        (shape((experts, rows), F32), shape((2, rows, 128), F32), shape((2, rows, 128), F32)),
        "vv",
    )(routes.T, route_weight.T)
    parts = ring_exchange(packed, True)
    parts = ring_exchange(four_copies(parts), False).reshape(peers, rows + EXTRA, chans)
    part = capacity // CHUNKS
    stream, gains, *sent = call(
        stream_kernel,
        (shape((rows, chans)), shape((peers, chans), F32)) + (shape((experts, part, chans)),) * CHUNKS,
        "vvvv",
        [
            vmem((2 * peers, rows), F32),
            vmem((rows, width), F32),
            vmem((rows, width)),
            vmem((slots, rows)),
        ],
        mib=16,
    )(parts, out_weight, residual_in, rank)
    half = slots // CHUNKS // 2
    returned = []
    for c in range(CHUNKS):
        received = exchange(sent[c], "sp")
        halves = received.reshape(1, 2, half, chans)
        outbound = jnp.broadcast_to(halves, (2, 2, half, chans)).reshape(4, half, chans)
        gathered = ring_exchange(outbound, True)
        gathered = ring_exchange(four_copies(gathered), False).reshape(peers, half, chans)
        partial = call(
            expert_kernel,
            shape((peers, half, chans)),
            "vvhhhhhh",
            [vmem((half, width))]
            + [vmem(gate_a.shape), vmem(up_a.shape), vmem(down_a.shape)] * 2,
            copies=6,
            mib=20,
        )(gathered, gains, gate_a, up_a, down_a, gate_b, up_b, down_b)
        pieces = ring_exchange(partial.reshape(4, 4, half, chans), False)
        summed = jnp.sum(pieces.astype(F32), 0).astype(BF16)
        pieces = ring_exchange(summed, True).reshape(2, 2, half, chans)
        summed = jnp.sum(pieces.astype(F32), 0).astype(BF16)
        back = exchange(summed.reshape(experts, part, chans), "sp")
        returned.append(back.reshape(2 * half, chans))
    return call(mix_kernel, shape((rows, chans)), "v" * (CHUNKS + 3))(
        *returned, pick, weight, stream
    )


def solution(mesh):
    split = Mesh(mesh.devices.reshape(mesh.shape["sp"], 4, 4), ("sp", "tp_0", "tp_1"))
    in_specs = (
        P("sp", TP),
        P("sp", TP),
        P("sp", TP),
        P("sp"),
        P(None, TP),
        P(TP),
        P(None, TP),
        P(TP),
        P("sp", None),
        P("sp", None),
        P("sp", None, TP),
        P("sp", None, TP),
        P("sp", TP, None),
    )
    out_specs = P("sp", TP)
    return jax.shard_map(
        per_device, mesh=split, in_specs=in_specs, out_specs=out_specs, check_vma=False
    )
```

```python
import jax
import jax.numpy as jnp
from jax import lax
from jax.experimental import pallas as pl
from jax.experimental.pallas import tpu as pltpu
from jax.sharding import Mesh
from jax.sharding import PartitionSpec as P


TP = ("tp_0", "tp_1")
epsilon = 1e-06
F32 = jnp.float32
BF16 = jnp.bfloat16
HALO = 32
CHUNKS = 1
EXTRA = 16


def vmem(dims, dtype=BF16):
    return pltpu.VMEM(dims, dtype)


def call(kernel, outs, ins, scratch=(), copies=0, spread=False, mib=4, flops=0):
    space = {"h": pltpu.HBM, "v": pltpu.VMEM}
    sems = [pltpu.SemaphoreType.DMA((copies,))] if copies else []
    out_space = pltpu.HBM if spread else pltpu.VMEM
    return pl.pallas_call(
        kernel,
        out_shape=outs,
        in_specs=[pl.BlockSpec(memory_space=space[c]) for c in ins],
        out_specs=jax.tree.map(lambda _: pl.BlockSpec(memory_space=out_space), outs),
        scratch_shapes=list(scratch) + sems,
        cost_estimate=pl.CostEstimate(flops=flops, bytes_accessed=0, transcendentals=0),
        compiler_params=pltpu.CompilerParams(vmem_limit_bytes=mib * 2**20),
    )


def start(pairs, sems, first=0):
    made = [
        pltpu.make_async_copy(src, dst, sems.at[first + i]) for i, (src, dst) in enumerate(pairs)
    ]
    for copy in made:
        copy.start()
    return made


def finish(made):
    for copy in made:
        copy.wait()


def place_of(core, peer):
    return jnp.where(core == 0, peer, (peer % 4) * 4 + peer // 4)


def shape(dims, dtype=BF16):
    return jax.ShapeDtypeStruct(dims, dtype)


def down_lanes(row):
    return jnp.concatenate(
        [
            jnp.transpose(jnp.broadcast_to(row[:, i : i + 128], (128, 128)))
            for i in range(0, row.shape[1], 128)
        ],
        0,
    )


def gate_of(value, gate):
    return (value.astype(F32) * jax.nn.sigmoid(gate.astype(F32))).astype(BF16)


def conv_kernel(halo, gated, docs, consts, sent, gext, dext, out, sems):
    rows, chans = gated.shape
    ntaps = consts.shape[0] - 2
    gext[:HALO] = halo[:HALO].astype(F32)
    gext[HALO:] = gated[...].astype(F32)
    dext[:HALO] = halo[HALO:].astype(F32)
    dext[HALO:] = docs[...].astype(F32)
    kernel = consts[...].astype(F32)
    first = HALO - ntaps + 1
    step = 64
    means = []
    for r in range(0, rows, step):
        doc = dext[HALO + r : HALO + r + step]
        acc = jnp.zeros((step, chans), F32)
        for j in range(ntaps):
            at = first + j + r
            acc = acc + jnp.where(
                dext[at : at + step] == doc, gext[at : at + step] * kernel[j : j + 1], 0.0
            )
        mean = jnp.mean(acc, 1, keepdims=True)
        out[r : r + step] = (acc - mean).astype(BF16)
        means.append(jnp.broadcast_to(mean, (step, 128)))
    lines = []
    for i in range(rows // 128):
        lines.append(jnp.transpose(jnp.concatenate(means[2 * i : 2 * i + 2], 0))[:1])
    mean = jnp.concatenate(lines, 0)
    high = mean.astype(BF16).astype(F32)
    low = mean - high
    tail = jnp.concatenate([high, low, kernel[ntaps:]], 0)
    tail = jnp.concatenate([tail, jnp.zeros((EXTRA - tail.shape[0], 128), F32)], 0)
    out[rows:] = tail.astype(BF16)
    finish(start([(out, sent.at[i]) for i in range(sent.shape[0])], sems))


def routing_kernel(routes, weights, rank_out, pick_out, weight_out):
    rows = routes.shape[1]
    experts = rank_out.shape[0]
    part = 4 * rows // experts // CHUNKS
    expert = lax.broadcasted_iota(jnp.int32, (experts, rows), 0)
    first = routes[:1] == expert
    second = routes[1:] == expert
    named = jnp.logical_or(first, second)
    before = lax.broadcasted_iota(jnp.int32, (rows, rows), 0) < lax.broadcasted_iota(
        jnp.int32, (rows, rows), 1
    )
    rank = jnp.dot(
        named.astype(F32).astype(BF16),
        before.astype(F32).astype(BF16),
        preferred_element_type=F32,
    )
    rank_out[...] = jnp.where(named, rank, -1.0)
    slot = rank + (expert * part).astype(F32)
    for c in range(1, CHUNKS):
        slot = slot + jnp.where(rank >= c * part, float((experts - 1) * part), 0.0)
    for k, chosen in enumerate((first, second)):
        pick = jnp.sum(jnp.where(chosen, slot, 0.0), 0, keepdims=True)
        pick_out[k] = down_lanes(pick)
        weight_out[k] = down_lanes(weights[k : k + 1])


def stream_kernel(parts, out_weight, residual, rank, stream_out, gains, *rest):
    sent, (means, full, act, place) = rest[:CHUNKS], rest[CHUNKS:]
    peers, extended, chans = parts.shape
    rows = extended - EXTRA
    width = peers * chans
    for d in range(peers):
        tail = parts[d, rows:].astype(F32)
        gains[d : d + 1] = tail[2 * (rows // 128) + 1 : 2 * (rows // 128) + 2]
        for i in range(rows // 128):
            means[d : d + 1, 128 * i : 128 * (i + 1)] = tail[i : i + 1]
            means[peers + d : peers + d + 1, 128 * i : 128 * (i + 1)] = tail[
                rows // 128 + i : rows // 128 + i + 1
            ]
    owner = lax.broadcasted_iota(jnp.int32, (2 * peers, width), 0)
    block = lax.broadcasted_iota(jnp.int32, (2 * peers, width), 1) // chans
    spread = jnp.logical_or(owner == block, owner == block + peers).astype(F32).astype(BF16)
    full[...] = lax.dot_general(
        means[...].astype(BF16),
        spread,
        (((0,), (0,)), ((), ())),
        preferred_element_type=F32,
    )
    nextra = 2 * (rows // 128)
    step = 64
    for r in range(0, rows, step):
        total = jnp.zeros((step, chans), F32)
        square = jnp.zeros((step, chans), F32)
        for d in range(peers):
            x = full[r : r + step, d * chans : (d + 1) * chans] + parts[
                d, r : r + step
            ].astype(F32)
            full[r : r + step, d * chans : (d + 1) * chans] = x
            total = total + x
            square = square + x * x
        mean = jnp.sum(total, 1, keepdims=True) / width
        var = jnp.sum(square, 1, keepdims=True) / width - mean * mean
        scale = lax.rsqrt(var + epsilon)
        for d in range(peers):
            gain = parts[d, rows:].astype(F32)[nextra : nextra + 1]
            x = full[r : r + step, d * chans : (d + 1) * chans]
            x = (x - mean) * scale * gain
            act[r : r + step, d * chans : (d + 1) * chans] = (x / (1.0 + jnp.exp(-x))).astype(BF16)
    projected = jnp.dot(act[...], out_weight[...], preferred_element_type=F32).astype(BF16)
    stream = (residual[...].astype(F32) + projected.astype(F32)).astype(BF16)
    stream_out[...] = stream
    experts, part, _ = sent[0].shape
    slots = experts * part
    slot = lax.broadcasted_iota(jnp.int32, (part, rows), 0)
    for c in range(CHUNKS):
        wanted = (slot + c * part).astype(F32)
        for e in range(experts):
            at = c * slots + e * part
            place[at : at + part] = (rank[e : e + 1] == wanted).astype(F32).astype(BF16)
    moved = jnp.dot(place[...], stream, preferred_element_type=F32).astype(BF16)
    for c in range(CHUNKS):
        sent[c][...] = moved[c * slots : (c + 1) * slots].reshape(sent[c].shape)


def expert_kernel(
    parts,
    gains,
    gate_ah,
    up_ah,
    down_ah,
    gate_bh,
    up_bh,
    down_bh,
    out,
    normed,
    gate_a,
    up_a,
    down_a,
    gate_b,
    up_b,
    down_b,
    sems,
):
    made = start(
        [
            (gate_ah, gate_a),
            (up_ah, up_a),
            (gate_bh, gate_b),
            (up_bh, up_b),
            (down_ah, down_a),
            (down_bh, down_b),
        ],
        sems,
    )
    core = lax.axis_index("sp") % 2
    peers, rows, chans = parts.shape
    width = peers * chans
    step = 64
    for r in range(0, rows, step):
        square = jnp.zeros((step, chans), F32)
        for d in range(peers):
            x = parts[d, r : r + step].astype(F32)
            square = square + x * x
        scale = lax.rsqrt(jnp.sum(square, 1, keepdims=True) / width + epsilon)
        for d in range(peers):
            x = parts[place_of(core, d), r : r + step].astype(F32) * scale * gains[d : d + 1]
            normed[r : r + step, d * chans : (d + 1) * chans] = x.astype(BF16)
    finish(made)
    step = 256
    for r in range(0, rows, step):
        x = normed[r : r + step]
        hidden = []
        for gate_w, up_w in ((gate_a, up_a), (gate_b, up_b)):
            gate = jnp.dot(x, gate_w[...], preferred_element_type=F32)
            up = jnp.dot(x, up_w[...], preferred_element_type=F32)
            hidden.append((gate / (1.0 + jnp.exp(-gate)) * up).astype(BF16))
        for c in range(0, width, 512):
            y = jnp.dot(hidden[0], down_a[:, c : c + 512], preferred_element_type=F32)
            y = y + jnp.dot(hidden[1], down_b[:, c : c + 512], preferred_element_type=F32)
            y = y.astype(BF16)
            for i in range(512 // chans):
                out[place_of(core, c // chans + i), r : r + step] = y[:, i * chans : (i + 1) * chans]


def mix_kernel(*refs):
    returned, (pick, weight, stream, out) = refs[:CHUNKS], refs[CHUNKS:]
    rows = stream.shape[0]
    slots = returned[0].shape[0]
    lane = lax.broadcasted_iota(jnp.int32, (rows, 128), 1).astype(F32)
    routed = jnp.zeros(stream.shape, F32)
    for k in range(2):
        picked = jnp.zeros(stream.shape, F32)
        for c in range(CHUNKS):
            choose = jnp.concatenate(
                [
                    (pick[k] == lane + float(c * slots + s)).astype(F32).astype(BF16)
                    for s in range(0, slots, 128)
                ],
                1,
            )
            picked = picked + jnp.dot(choose, returned[c][...], preferred_element_type=F32)
        routed = routed + picked * weight[k]
    out[...] = (stream[...].astype(F32) + routed).astype(BF16)


def exchange(x, axis):
    return lax.all_to_all(x, axis, split_axis=0, concat_axis=0, tiled=True)


def rings(first):
    groups = []
    for s in range(lax.axis_size("sp")):
        along_x = (s % 2 == 0) == first
        for a in range(4):
            groups.append([s * 16 + (4 * a + b if along_x else 4 * b + a) for b in range(4)])
    return groups


def ring_exchange(x, first):
    return lax.all_to_all(
        x, ("sp", *TP), split_axis=0, concat_axis=0, axis_index_groups=rings(first), tiled=True
    )


def four_copies(x):
    return jnp.broadcast_to(x, (4, *x.shape))


def swap_pair(x):
    groups, peers = lax.axis_size("sp"), lax.axis_size(TP)
    pairs = [
        (s * peers + t, s * peers + (t ^ (1 if s % 2 == 0 else 4)))
        for s in range(groups)
        for t in range(peers)
    ]
    return lax.ppermute(x, ("sp", *TP), pairs)


def per_device(
    residual_in,
    conv_value,
    conv_gate,
    doc_ids,
    conv_kernel_w,
    ln_gain,
    out_weight,
    norm_gain,
    routes,
    route_weight,
    gate_w,
    up_w,
    down_w,
):
    rows, chans = conv_value.shape
    experts = lax.axis_size("sp")
    peers = lax.axis_size(TP)
    capacity = 4 * rows // experts
    slots = experts * capacity
    width = peers * chans
    gate_a, up_a, down_a = gate_w[0], up_w[0], down_w[0]

    gated = gate_of(conv_value, conv_gate)
    docs = jnp.broadcast_to(doc_ids.astype(BF16)[:, None], (rows, chans))
    consts = jnp.concatenate([conv_kernel_w, ln_gain[None], norm_gain[None]], 0)
    tail = jnp.concatenate(
        [
            gate_of(conv_value[rows - HALO :], conv_gate[rows - HALO :]),
            jnp.broadcast_to(doc_ids[rows - HALO :].astype(BF16)[:, None], (HALO, chans)),
        ],
        0,
    )
    n = lax.axis_size("sp")
    halo = lax.ppermute(tail, "sp", [(i, i + 1) for i in range(n - 1)])
    gate_b = swap_pair(gate_a)
    up_b = swap_pair(up_a)
    down_b = swap_pair(down_a)
    packed = call(
        conv_kernel,
        shape((peers, rows + EXTRA, chans)),
        "vvvv",
        [
            vmem((rows + HALO, chans), F32),
            vmem((rows + HALO, chans), F32),
            vmem((rows + EXTRA, chans)),
        ],
        copies=peers,
        spread=True,
    )(halo, gated, docs, consts)
    rank, pick, weight = call(
        routing_kernel,
        (shape((experts, rows), F32), shape((2, rows, 128), F32), shape((2, rows, 128), F32)),
        "vv",
    )(routes.T, route_weight.T)
    parts = exchange(packed, TP)
    part = capacity // CHUNKS
    stream, gains, *sent = call(
        stream_kernel,
        (shape((rows, chans)), shape((peers, chans), F32)) + (shape((experts, part, chans)),) * CHUNKS,
        "vvvv",
        [
            vmem((2 * peers, rows), F32),
            vmem((rows, width), F32),
            vmem((rows, width)),
            vmem((slots, rows)),
        ],
        mib=16,
    )(parts, out_weight, residual_in, rank)
    half = slots // CHUNKS // 2
    returned = []
    for c in range(CHUNKS):
        received = exchange(sent[c], "sp")
        halves = received.reshape(1, 2, half, chans)
        outbound = jnp.broadcast_to(halves, (2, 2, half, chans)).reshape(4, half, chans)
        gathered = ring_exchange(outbound, True)
        gathered = ring_exchange(four_copies(gathered), False).reshape(peers, half, chans)
        partial = call(
            expert_kernel,
            shape((peers, half, chans)),
            "vvhhhhhh",
            [vmem((half, width))]
            + [vmem(gate_a.shape), vmem(up_a.shape), vmem(down_a.shape)] * 2,
            copies=6,
            mib=20,
        )(gathered, gains, gate_a, up_a, down_a, gate_b, up_b, down_b)
        pieces = ring_exchange(partial.reshape(4, 4, half, chans), False)
        summed = jnp.sum(pieces.astype(F32), 0).astype(BF16)
        pieces = ring_exchange(summed, True).reshape(2, 2, half, chans)
        summed = jnp.sum(pieces.astype(F32), 0).astype(BF16)
        back = exchange(summed.reshape(experts, part, chans), "sp")
        returned.append(back.reshape(2 * half, chans))
    return call(mix_kernel, shape((rows, chans)), "v" * (CHUNKS + 3))(
        *returned, pick, weight, stream
    )


def solution(mesh):
    split = Mesh(mesh.devices.reshape(mesh.shape["sp"], 4, 4), ("sp", "tp_0", "tp_1"))
    in_specs = (
        P("sp", TP),
        P("sp", TP),
        P("sp", TP),
        P("sp"),
        P(None, TP),
        P(TP),
        P(None, TP),
        P(TP),
        P("sp", None),
        P("sp", None),
        P("sp", None, TP),
        P("sp", None, TP),
        P("sp", TP, None),
    )
    out_specs = P("sp", TP)
    return jax.shard_map(
        per_device, mesh=split, in_specs=in_specs, out_specs=out_specs, check_vma=False
    )
```

```python
import functools

import jax
import jax.numpy as jnp
from jax import lax
from jax.experimental import pallas as pl
from jax.experimental.pallas import tpu as pltpu
from jax.sharding import Mesh
from jax.sharding import PartitionSpec as P


TP = ("tp_0", "tp_1")
epsilon = 1e-06
F32 = jnp.float32
BF16 = jnp.bfloat16
HALO = 32
CHUNKS = 1
RING = 4
RELAYS = {"gate": ((1, 1),), "up": ((2, -1),), "down": ()}
EXTRA = 16


def vmem(dims, dtype=BF16):
    return pltpu.VMEM(dims, dtype)


def call(kernel, outs, ins, scratch=(), copies=0, spread=False, mib=4, flops=0):
    space = {"h": pltpu.HBM, "v": pltpu.VMEM}
    sems = [pltpu.SemaphoreType.DMA((copies,))] if copies else []
    out_space = pltpu.HBM if spread else pltpu.VMEM
    return pl.pallas_call(
        kernel,
        out_shape=outs,
        in_specs=[pl.BlockSpec(memory_space=space[c]) for c in ins],
        out_specs=jax.tree.map(lambda _: pl.BlockSpec(memory_space=out_space), outs),
        scratch_shapes=list(scratch) + sems,
        cost_estimate=pl.CostEstimate(flops=flops, bytes_accessed=0, transcendentals=0),
        compiler_params=pltpu.CompilerParams(vmem_limit_bytes=mib * 2**20),
    )


def start(pairs, sems, first=0):
    made = [
        pltpu.make_async_copy(src, dst, sems.at[first + i]) for i, (src, dst) in enumerate(pairs)
    ]
    for copy in made:
        copy.start()
    return made


def finish(made):
    for copy in made:
        copy.wait()


def ring_place(core, peer):
    return jnp.where(core == 0, peer % 4, peer // 4)


def shape(dims, dtype=BF16):
    return jax.ShapeDtypeStruct(dims, dtype)


def down_lanes(row):
    return jnp.concatenate(
        [
            jnp.transpose(jnp.broadcast_to(row[:, i : i + 128], (128, 128)))
            for i in range(0, row.shape[1], 128)
        ],
        0,
    )


def gate_of(value, gate):
    return (value.astype(F32) * jax.nn.sigmoid(gate.astype(F32))).astype(BF16)


def conv_kernel(halo, gated, docs, consts, sent, gext, dext, out, sems):
    rows, chans = gated.shape
    ntaps = consts.shape[0] - 2
    gext[:HALO] = halo[:HALO].astype(F32)
    gext[HALO:] = gated[...].astype(F32)
    dext[:HALO] = halo[HALO:].astype(F32)
    dext[HALO:] = docs[...].astype(F32)
    kernel = consts[...].astype(F32)
    first = HALO - ntaps + 1
    step = 64
    means = []
    for r in range(0, rows, step):
        doc = dext[HALO + r : HALO + r + step]
        acc = jnp.zeros((step, chans), F32)
        for j in range(ntaps):
            at = first + j + r
            acc = acc + jnp.where(
                dext[at : at + step] == doc, gext[at : at + step] * kernel[j : j + 1], 0.0
            )
        mean = jnp.mean(acc, 1, keepdims=True)
        out[r : r + step] = (acc - mean).astype(BF16)
        means.append(jnp.broadcast_to(mean, (step, 128)))
    lines = []
    for i in range(rows // 128):
        lines.append(jnp.transpose(jnp.concatenate(means[2 * i : 2 * i + 2], 0))[:1])
    mean = jnp.concatenate(lines, 0)
    high = mean.astype(BF16).astype(F32)
    low = mean - high
    tail = jnp.concatenate([high, low, kernel[ntaps:]], 0)
    tail = jnp.concatenate([tail, jnp.zeros((EXTRA - tail.shape[0], 128), F32)], 0)
    out[rows:] = tail.astype(BF16)
    finish(start([(out, sent.at[i]) for i in range(sent.shape[0])], sems))


def ranks_of(routes, experts):
    rows = routes.shape[1]
    expert = lax.broadcasted_iota(jnp.int32, (experts, rows), 0)
    first = routes[:1] == expert
    second = routes[1:] == expert
    named = jnp.logical_or(first, second)
    before = lax.broadcasted_iota(jnp.int32, (rows, rows), 0) < lax.broadcasted_iota(
        jnp.int32, (rows, rows), 1
    )
    rank = jnp.dot(
        named.astype(F32).astype(BF16),
        before.astype(F32).astype(BF16),
        preferred_element_type=F32,
    )
    return expert, first, second, named, rank


def routing_kernel(routes, rank_out):
    _, _, _, named, rank = ranks_of(routes, rank_out.shape[0])
    rank_out[...] = jnp.where(named, rank, -1.0)


def picks_kernel(experts, routes, weights, pick_out, weight_out):
    rows = routes.shape[1]
    part = 4 * rows // experts // CHUNKS
    expert, first, second, _, rank = ranks_of(routes, experts)
    slot = rank + (expert * part).astype(F32)
    for c in range(1, CHUNKS):
        slot = slot + jnp.where(rank >= c * part, float((experts - 1) * part), 0.0)
    for k, chosen in enumerate((first, second)):
        pick = jnp.sum(jnp.where(chosen, slot, 0.0), 0, keepdims=True)
        pick_out[k] = down_lanes(pick)
        weight_out[k] = down_lanes(weights[k : k + 1])


def stream_kernel(parts, out_weight, residual, rank, stream_out, gains, *rest):
    sent, (means, full, act, place) = rest[:CHUNKS], rest[CHUNKS:]
    peers, extended, chans = parts.shape
    rows = extended - EXTRA
    width = peers * chans
    for d in range(peers):
        tail = parts[d, rows:].astype(F32)
        gains[d : d + 1] = tail[2 * (rows // 128) + 1 : 2 * (rows // 128) + 2]
        for i in range(rows // 128):
            means[d : d + 1, 128 * i : 128 * (i + 1)] = tail[i : i + 1]
            means[peers + d : peers + d + 1, 128 * i : 128 * (i + 1)] = tail[
                rows // 128 + i : rows // 128 + i + 1
            ]
    owner = lax.broadcasted_iota(jnp.int32, (2 * peers, width), 0)
    block = lax.broadcasted_iota(jnp.int32, (2 * peers, width), 1) // chans
    spread = jnp.logical_or(owner == block, owner == block + peers).astype(F32).astype(BF16)
    full[...] = lax.dot_general(
        means[...].astype(BF16),
        spread,
        (((0,), (0,)), ((), ())),
        preferred_element_type=F32,
    )
    nextra = 2 * (rows // 128)
    step = 64
    for r in range(0, rows, step):
        total = jnp.zeros((step, chans), F32)
        square = jnp.zeros((step, chans), F32)
        for d in range(peers):
            x = full[r : r + step, d * chans : (d + 1) * chans] + parts[
                d, r : r + step
            ].astype(F32)
            full[r : r + step, d * chans : (d + 1) * chans] = x
            total = total + x
            square = square + x * x
        mean = jnp.sum(total, 1, keepdims=True) / width
        var = jnp.sum(square, 1, keepdims=True) / width - mean * mean
        scale = lax.rsqrt(var + epsilon)
        for d in range(peers):
            gain = parts[d, rows:].astype(F32)[nextra : nextra + 1]
            x = full[r : r + step, d * chans : (d + 1) * chans]
            x = (x - mean) * scale * gain
            act[r : r + step, d * chans : (d + 1) * chans] = (x / (1.0 + jnp.exp(-x))).astype(BF16)
    projected = jnp.dot(act[...], out_weight[...], preferred_element_type=F32).astype(BF16)
    stream = (residual[...].astype(F32) + projected.astype(F32)).astype(BF16)
    stream_out[...] = stream
    experts, part, _ = sent[0].shape
    slots = experts * part
    slot = lax.broadcasted_iota(jnp.int32, (part, rows), 0)
    for c in range(CHUNKS):
        wanted = (slot + c * part).astype(F32)
        for e in range(experts):
            at = c * slots + e * part
            place[at : at + part] = (rank[e : e + 1] == wanted).astype(F32).astype(BF16)
    moved = jnp.dot(place[...], stream, preferred_element_type=F32).astype(BF16)
    for c in range(CHUNKS):
        sent[c][...] = moved[c * slots : (c + 1) * slots].reshape(sent[c].shape)


def spread_kernel(received, out, sems):
    core = lax.axis_index("sp") % 2
    peers, rows, _ = out.shape
    pairs = []
    for i in range(peers):
        first = pl.multiple_of(ring_place(core, i) * rows, rows)
        pairs.append((received.at[pl.ds(first, rows)], out.at[i]))
    finish(start(pairs, sems))


def expert_kernel(parts, gains, *refs):
    ways = RING
    gates_h, ups_h, downs_h = refs[:ways], refs[ways : 2 * ways], refs[2 * ways : 3 * ways + 1]
    out, normed, gate_w, up_w, down_w, hidden, sems = refs[3 * ways + 1 :]
    peers, rows, chans = parts.shape
    width = peers * chans
    units = gates_h[0].shape[1]
    pairs = []
    for i in range(ways):
        pairs.append((gates_h[i], gate_w.at[:, i * units : (i + 1) * units]))
        pairs.append((ups_h[i], up_w.at[:, i * units : (i + 1) * units]))
    at = 0
    for ref in downs_h:
        pairs.append((ref, down_w.at[at : at + ref.shape[0]]))
        at += ref.shape[0]
    made = start(pairs, sems)
    step = 64
    for r in range(0, rows, step):
        square = jnp.zeros((step, chans), F32)
        for d in range(peers):
            x = parts[d, r : r + step].astype(F32)
            square = square + x * x
        scale = lax.rsqrt(jnp.sum(square, 1, keepdims=True) / width + epsilon)
        for d in range(peers):
            x = parts[d, r : r + step].astype(F32) * scale * gains[d : d + 1]
            normed[r : r + step, d * chans : (d + 1) * chans] = x.astype(BF16)
    for i in range(ways):
        finish(made[2 * i : 2 * i + 2])
        cols = slice(i * units, (i + 1) * units)
        gate = jnp.dot(normed[...], gate_w[:, cols], preferred_element_type=F32)
        up = jnp.dot(normed[...], up_w[:, cols], preferred_element_type=F32)
        hidden[:, cols] = (gate / (1.0 + jnp.exp(-gate)) * up).astype(BF16)
    finish(made[2 * ways :])
    for c in range(0, width, 512):
        y = jnp.dot(hidden[...], down_w[:, c : c + 512], preferred_element_type=F32).astype(BF16)
        for i in range(512 // chans):
            out[c // chans + i] = y[:, i * chans : (i + 1) * chans]


def sum_kernel(pieces, out):
    core = lax.axis_index("sp") % 2
    rows = pieces.shape[1]
    for r in range(RING):
        total = jnp.zeros(pieces.shape[1:], F32)
        for k in range(RING):
            total = total + pieces[jnp.where(core == 0, RING * k + r, RING * r + k)].astype(F32)
        out[r * rows : (r + 1) * rows] = total.astype(BF16)


def mix_kernel(*refs):
    returned, (pick, weight, stream, out) = refs[:CHUNKS], refs[CHUNKS:]
    rows = stream.shape[0]
    slots = returned[0].shape[0]
    lane = lax.broadcasted_iota(jnp.int32, (rows, 128), 1).astype(F32)
    routed = jnp.zeros(stream.shape, F32)
    for k in range(2):
        picked = jnp.zeros(stream.shape, F32)
        for c in range(CHUNKS):
            choose = jnp.concatenate(
                [
                    (pick[k] == lane + float(c * slots + s)).astype(F32).astype(BF16)
                    for s in range(0, slots, 128)
                ],
                1,
            )
            picked = picked + jnp.dot(choose, returned[c][...], preferred_element_type=F32)
        routed = routed + picked * weight[k]
    out[...] = (stream[...].astype(F32) + routed).astype(BF16)


def exchange(x, axis):
    return lax.all_to_all(x, axis, split_axis=0, concat_axis=0, tiled=True)


def from_ring(x, by):
    pairs = []
    for s in range(lax.axis_size("sp")):
        for t in range(16):
            y, x_ = t // 4, t % 4
            to = 4 * y + (x_ + by) % 4 if s % 2 == 0 else 4 * ((y + by) % 4) + x_
            pairs.append((16 * s + t, 16 * s + to))
    return lax.ppermute(x, ("sp", *TP), pairs)


def per_device(
    residual_in,
    conv_value,
    conv_gate,
    doc_ids,
    conv_kernel_w,
    ln_gain,
    out_weight,
    norm_gain,
    routes,
    route_weight,
    gate_w,
    up_w,
    down_w,
):
    rows, chans = conv_value.shape
    experts = lax.axis_size("sp")
    peers = lax.axis_size(TP)
    capacity = 4 * rows // experts
    slots = experts * capacity
    width = peers * chans
    gate_a, up_a, down_a = gate_w[0], up_w[0], down_w[0]

    gated = gate_of(conv_value, conv_gate)
    docs = jnp.broadcast_to(doc_ids.astype(BF16)[:, None], (rows, chans))
    consts = jnp.concatenate([conv_kernel_w, ln_gain[None], norm_gain[None]], 0)
    tail = jnp.concatenate(
        [
            gate_of(conv_value[rows - HALO :], conv_gate[rows - HALO :]),
            jnp.broadcast_to(doc_ids[rows - HALO :].astype(BF16)[:, None], (HALO, chans)),
        ],
        0,
    )
    n = lax.axis_size("sp")
    halo = lax.ppermute(tail, "sp", [(i, i + 1) for i in range(n - 1)])
    blocks = {"gate": [gate_a], "up": [up_a], "down": [down_a]}
    for name, found in blocks.items():
        for source, by in ((0, 1), (0, -1)) + RELAYS[name]:
            found.append(from_ring(found[source], by))
    found = blocks["down"]
    middle = down_a.shape[0] // 2
    found.append(from_ring(found[1][:middle], 1))
    found.append(from_ring(found[2][middle:], -1))
    packed = call(
        conv_kernel,
        shape((peers, rows + EXTRA, chans)),
        "vvvv",
        [
            vmem((rows + HALO, chans), F32),
            vmem((rows + HALO, chans), F32),
            vmem((rows + EXTRA, chans)),
        ],
        copies=peers,
        spread=True,
    )(halo, gated, docs, consts)
    rank = call(routing_kernel, shape((experts, rows), F32), "v")(routes.T)
    pick, weight = call(
        functools.partial(picks_kernel, experts),
        (shape((2, rows, 128), F32), shape((2, rows, 128), F32)),
        "vv",
    )(routes.T, route_weight.T)
    parts = exchange(packed, TP)
    part = capacity // CHUNKS
    stream, gains, *sent = call(
        stream_kernel,
        (shape((rows, chans)), shape((peers, chans), F32)) + (shape((experts, part, chans)),) * CHUNKS,
        "vvvv",
        [
            vmem((2 * peers, rows), F32),
            vmem((rows, width), F32),
            vmem((rows, width)),
            vmem((slots, rows)),
        ],
        mib=16,
    )(parts, out_weight, residual_in, rank)
    quarter = slots // CHUNKS // RING
    returned = []
    for c in range(CHUNKS):
        received = exchange(sent[c], "sp")
        outbound = call(
            spread_kernel, shape((peers, quarter, chans)), "v", copies=peers, spread=True
        )(received.reshape(RING * quarter, chans))
        gathered = exchange(outbound, TP)
        units = gate_a.shape[1]
        partial = call(
            expert_kernel,
            shape((peers, quarter, chans)),
            "vv" + "h" * (3 * RING + 1),
            [
                vmem((quarter, width)),
                vmem((width, RING * units)),
                vmem((width, RING * units)),
                vmem((RING * units, width)),
                vmem((quarter, RING * units)),
            ],
            copies=3 * RING + 1,
            mib=24,
        )(gathered, gains, *blocks["gate"], *blocks["up"], *blocks["down"])
        pieces = exchange(partial, TP)
        summed = call(sum_kernel, shape((RING * quarter, chans)), "v")(pieces)
        back = exchange(summed.reshape(experts, part, chans), "sp")
        returned.append(back.reshape(RING * quarter, chans))
    return call(mix_kernel, shape((rows, chans)), "v" * (CHUNKS + 3))(
        *returned, pick, weight, stream
    )


def solution(mesh):
    split = Mesh(mesh.devices.reshape(mesh.shape["sp"], 4, 4), ("sp", "tp_0", "tp_1"))
    in_specs = (
        P("sp", TP),
        P("sp", TP),
        P("sp", TP),
        P("sp"),
        P(None, TP),
        P(TP),
        P(None, TP),
        P(TP),
        P("sp", None),
        P("sp", None),
        P("sp", None, TP),
        P("sp", None, TP),
        P("sp", TP, None),
    )
    out_specs = P("sp", TP)
    return jax.shard_map(
        per_device, mesh=split, in_specs=in_specs, out_specs=out_specs, check_vma=False
    )
```
